32 devices in a mesh: sp: 8 (over z, y), tp: 4 (over x, core).
Axes of the slice: x: 2, y: 2, z: 4, core: 2. Of those that a mesh axis runs over, the one named last changes fastest.
Arguments:
- tokens: bfloat16 [6144, 2048], P('sp', 'tp'), may hold values from -6 to 6
- norm_gain: float32 [2048], replicated, may hold values from 0.1 to 1.9
- w_query: bfloat16 [2048, 2048], P(None, 'tp'), may hold values from -4 to 4
- w_key: bfloat16 [2048, 2048], P(None, 'tp'), may hold values from -4 to 4
- w_value: bfloat16 [2048, 2048], P(None, 'tp'), may hold values from -0.125 to 0.125
- w_outer: bfloat16 [2048, 2048], P(None, 'tp'), may hold values from -0.125 to 0.125
- w_inner: bfloat16 [2048, 2048], P(None, 'tp'), may hold values from -0.125 to 0.125
- w_signal: bfloat16 [2048, 2048], P(None, 'tp'), may hold values from -0.125 to 0.125
- conv_taps: bfloat16 [3, 2048], P(None, 'tp'), may hold values from -3.5 to 3.5
- lambdas: float32 [8], P('tp'), may hold values from 0.3 to 0.8
- head_gain: float32 [256], replicated, may hold values from 0.1 to 1.9
- attend_proj: bfloat16 [2048, 2048], P('tp'), may hold values from -0.125 to 0.125
- convolve_proj: bfloat16 [2048, 2048], P('tp'), may hold values from -0.125 to 0.125
Outputs:
- mixed: bfloat16 [6144, 2048], P(('sp', 'tp'))
- row_lse: float32 [6144, 16], P('sp', 'tp')
The draws below stay inside these ranges and needn't reach their ends.
All inputs are finite; a program needn't handle non-finite values.
Results may differ from the reference program's by a relative error of at most 0.015.
Values may be sent and summed in bfloat16 or wider, within the bound.
A program may use at most 128 MiB of HBM per device.

```python
import math
import jax
import jax.numpy as jnp
from jax import lax

D = 2048
HEADS = 8
HEAD_DIM = 128
CONV = 2048
TOK_DEV = 768
TOKENS = 6144
N_TP = 4


def query_key_pair(key):
    width = 2 * HEADS * HEAD_DIM
    spread = 1.3 / math.sqrt(D)
    key_part = jax.random.normal(jax.random.fold_in(key, 701), (D, width), jnp.float32) * spread
    noise_part = jax.random.normal(jax.random.fold_in(key, 702), (D, width), jnp.float32) * spread
    query_part = noise_part
    return (jnp.clip(query_part, -4.0, 4.0), jnp.clip(key_part, -4.0, 4.0))


def draw_w_query(key, part):
    return query_key_pair(key)[0].astype(jnp.bfloat16)


def draw_w_key(key, part):
    return query_key_pair(key)[1].astype(jnp.bfloat16)


def level_of(rng, dims, cuts, least, top_value):
    def one(position, parts):
        heights = jax.random.uniform(jax.random.fold_in(jax.random.fold_in(rng, 6), position), (parts,), jnp.float32, least / len(cuts), top_value / len(cuts))
        return jnp.repeat(jnp.exp(heights), dims[position] // parts).reshape((-1,) + (1,) * (len(dims) - position - 1))

    loudness = one(*cuts[0])
    for cut in cuts[1:]:
        loudness = loudness * one(*cut)
    return loudness


def bell_draw(rng, shape, scale, limit, pieces=(), kind=jnp.bfloat16):
    level = level_of(rng, shape, pieces, -0.22, 0.18) if pieces else 1.0
    entries = jax.random.normal(rng, shape, jnp.float32) * scale * level
    return jnp.minimum(jnp.maximum(entries, -limit), limit).astype(kind)


def setup_inputs(seed: int = 0) -> dict:
    keys = jax.random.split(jax.random.key(seed), 14)
    return {
        "tokens": bell_draw(keys[0], (TOKENS, D), 1.0, 6.0, ((0, 8), (1, 4))),
        "norm_gain": jnp.clip(1.0 + 0.18 * jax.random.normal(keys[1], (D,), jnp.float32), 0.1, 1.9),
        "w_query": draw_w_query(jax.random.fold_in(keys[13], 71), 0),
        "w_key": draw_w_key(jax.random.fold_in(keys[13], 71), 0),
        "w_value": bell_draw(keys[4], (D, 2 * HEADS * HEAD_DIM), D ** -0.5, 0.125, ((1, 4),)),
        "w_outer": bell_draw(keys[5], (D, CONV), D ** -0.5, 0.125, ((1, 4),)),
        "w_inner": bell_draw(keys[6], (D, CONV), D ** -0.5, 0.125, ((1, 4),)),
        "w_signal": bell_draw(keys[7], (D, CONV), D ** -0.5, 0.125, ((1, 4),)),
        "conv_taps": bell_draw(keys[8], (3, CONV), 3 ** -0.5, 3.5, ((1, 4),)),
        "lambdas": jnp.clip(0.3 + 0.5 * jax.random.uniform(keys[9], (HEADS,), jnp.float32) ** level_of(keys[9], (HEADS,), ((0, 4),), -0.2, 0.2), 0.3, 0.8),
        "head_gain": jnp.clip(1.0 + 0.18 * jax.random.normal(keys[10], (2 * HEAD_DIM,), jnp.float32), 0.1, 1.9),
        "attend_proj": bell_draw(keys[11], (2 * HEADS * HEAD_DIM, D), (2 * HEADS * HEAD_DIM) ** -0.5, 0.125, ((0, 4),)),
        "convolve_proj": bell_draw(keys[12], (CONV, D), CONV ** -0.5, 0.125, ((0, 4),)),
    }


ROPE_BASE = 500000.0
NORM_EPS = 1e-05
HEAD_KEEP = 0.8
MASKED = -1e+30

def rotate(values_in, positions):
    half_width = values_in.shape[-1] // 2
    inverse = ROPE_BASE ** (-jnp.arange(half_width, dtype=jnp.float32) * 2.0 / values_in.shape[-1])
    angles = positions.astype(jnp.float32)[:, None] * inverse[None, :]
    cosine = jnp.cos(angles)[:, None, :]
    sine_part = jnp.sin(angles)[:, None, :]
    first_half = values_in[..., :half_width]
    second_half = values_in[..., half_width:]
    return jnp.concatenate([first_half * cosine - second_half * sine_part, second_half * cosine + first_half * sine_part], axis=-1)

def reference(tokens, norm_gain, w_query, w_key, w_value, w_outer, w_inner, w_signal, conv_taps, lambdas, head_gain, attend_proj, convolve_proj):
    row_count = tokens.shape[0]
    widened = tokens.astype(jnp.float32)
    scaled = (widened * norm_gain[None, :]).astype(jnp.bfloat16)
    inv_rms = lax.rsqrt(lax.optimization_barrier(jnp.mean(widened * widened, axis=1, keepdims=True)) + NORM_EPS)

    def project(weight):
        return inv_rms * jnp.dot(scaled, weight, preferred_element_type=jnp.float32)
    positions = jnp.arange(row_count, dtype=jnp.int32)
    queries = rotate(project(w_query).reshape(row_count, 2 * HEADS, HEAD_DIM), positions).astype(jnp.bfloat16)
    key_rows = rotate(project(w_key).reshape(row_count, 2 * HEADS, HEAD_DIM), positions).astype(jnp.bfloat16)
    value_rows = project(w_value).astype(jnp.bfloat16).reshape(row_count, HEADS, 2 * HEAD_DIM)
    block_count = row_count // TOK_DEV
    key_places = jnp.arange(row_count, dtype=jnp.int32)
    attended_heads = []
    lse_heads = []
    for head_index in range(HEADS):
        head_query = queries[:, 2 * head_index:2 * head_index + 2, :].astype(jnp.float32)
        head_key = key_rows[:, 2 * head_index:2 * head_index + 2, :].astype(jnp.float32)
        head_value = value_rows[:, head_index, :].astype(jnp.float32)
        head_lambda = lambdas[head_index]

        def one_block(block_index):
            first_row = block_index * TOK_DEV
            query_block = lax.dynamic_slice_in_dim(head_query, first_row, TOK_DEV, 0)
            scores = jnp.einsum('qjd,kjd->jqk', query_block, head_key) * HEAD_DIM ** (-0.5)
            query_places = first_row + jnp.arange(TOK_DEV, dtype=jnp.int32)
            allowed = key_places[None, :] <= query_places[:, None]
            scores = jnp.where(allowed[None], scores, MASKED)
            running_max = lax.optimization_barrier(jnp.max(scores, axis=2, keepdims=True))
            lifted = jnp.exp(scores - running_max)
            weight_sum = lax.optimization_barrier(jnp.sum(lifted, axis=2, keepdims=True))
            weights = lax.optimization_barrier((lifted / weight_sum).astype(jnp.bfloat16))
            mixed_pair = jnp.einsum('jqk,ke->jqe', weights.astype(jnp.float32), head_value)
            difference = mixed_pair[0] - head_lambda * mixed_pair[1]
            scale_back = lax.rsqrt(lax.optimization_barrier(jnp.mean(difference * difference, axis=1, keepdims=True)) + NORM_EPS)
            normed = (difference * scale_back * head_gain[None, :] * HEAD_KEEP).astype(jnp.bfloat16)
            log_sum = jnp.transpose((running_max + jnp.log(weight_sum))[:, :, 0], (1, 0))
            return (normed, log_sum)
        normed_blocks, lse_blocks = lax.map(one_block, jnp.arange(block_count, dtype=jnp.int32))
        attended_heads.append(normed_blocks.reshape(row_count, 2 * HEAD_DIM))
        lse_heads.append(lse_blocks.reshape(row_count, 2))
    attended = jnp.concatenate(attended_heads, axis=1)
    row_lse = jnp.concatenate(lse_heads, axis=1)
    product = project(w_inner) * project(w_signal)
    padded = jnp.concatenate([jnp.zeros((2, CONV), jnp.float32), product], axis=0)
    tap_values = conv_taps.astype(jnp.float32)
    smoothed = tap_values[0] * padded[:-2] + tap_values[1] * padded[1:-1] + tap_values[2] * padded[2:]
    convolved = (project(w_outer) * smoothed).astype(jnp.bfloat16)
    head_columns = HEADS // N_TP * 2 * HEAD_DIM
    channel_columns = CONV // N_TP
    summed = jnp.zeros((row_count, D), jnp.float32)
    for group_index in range(N_TP):
        head_lo = group_index * head_columns
        chan_lo = group_index * channel_columns
        partial_value = jnp.dot(attended[:, head_lo:head_lo + head_columns], attend_proj[head_lo:head_lo + head_columns], preferred_element_type=jnp.float32)
        partial_value = partial_value + jnp.dot(convolved[:, chan_lo:chan_lo + channel_columns], convolve_proj[chan_lo:chan_lo + channel_columns], preferred_element_type=jnp.float32)
        rounded = lax.optimization_barrier(partial_value.astype(jnp.bfloat16))
        summed = summed + rounded.astype(jnp.float32)
    return (summed.astype(jnp.bfloat16), row_lse)
```

```python
import functools
import math

import jax
import jax.numpy as jnp
from jax import lax
from jax.experimental import pallas as pl
from jax.experimental.pallas import tpu as pltpu
from jax.sharding import PartitionSpec as P

ROPE_BASE = 500000.0
NORM_EPS = 1e-05
HEAD_KEEP = 0.8
MASKED = -1e30
LOG2E = math.log2(math.e)
MESH = pl.DeviceIdType.MESH


def partner(value, axis, stride):
    return lax.ppermute(value, axis, [(i, i ^ 1 << stride) for i in range(lax.axis_size(axis))])


def passed_along(value, axis, steps):
    count = lax.axis_size(axis)
    initial, last = (max(0, -steps), min(count, count - steps))
    return lax.ppermute(value, axis, [(source, source + steps) for source in range(initial, last)])


def rotate(values_in, positions):
    half_width = values_in.shape[-1] // 2
    inverse = ROPE_BASE ** (-jnp.arange(half_width, dtype=jnp.float32) * 2.0 / values_in.shape[-1])
    angles = positions.astype(jnp.float32)[:, None] * inverse[None, :]
    cosine = jnp.cos(angles)[:, None, :]
    sine_part = jnp.sin(angles)[:, None, :]
    first_half = values_in[..., :half_width]
    second_half = values_in[..., half_width:]
    return jnp.concatenate(
        [
            first_half * cosine - second_half * sine_part,
            second_half * cosine + first_half * sine_part,
        ],
        axis=-1,
    )


def absorb(state, queries, positions, key_block, value_block, first_key):
    running_max, weight_sum, weighted = state
    head_count = weighted.shape[0]
    block_rows = key_block.shape[0]
    scores = jnp.einsum("qgd,kgd->gqk", queries, key_block, preferred_element_type=jnp.float32)
    scores = scores * queries.shape[-1] ** (-0.5)
    key_places = first_key + jnp.arange(block_rows, dtype=jnp.int32)
    allowed = key_places[None, :] <= positions[:, None]
    scores = jnp.where(allowed[None], scores, MASKED)
    scores = scores.reshape(head_count, 2, positions.shape[0], block_rows)
    raised = jnp.maximum(running_max, jnp.max(scores, axis=3))
    factor = jnp.exp(running_max - raised)
    lifted = jnp.exp(scores - raised[..., None])
    weight_sum = factor * weight_sum + jnp.sum(lifted, axis=3)
    values_here = value_block.reshape(block_rows, head_count, -1)
    weighted = factor[..., None] * weighted + jnp.einsum(
        "hjqk,khe->hjqe",
        lifted.astype(jnp.bfloat16),
        values_here,
        preferred_element_type=jnp.float32,
    )
    return (raised, weight_sum, weighted)


def empty_state(head_count, rows, head_width):
    return (
        jnp.full((head_count, 2, rows), MASKED, jnp.float32),
        jnp.zeros((head_count, 2, rows), jnp.float32),
        jnp.zeros((head_count, 2, rows, 2 * head_width), jnp.float32),
    )


def finish(state, lambdas, head_gain):
    running_max, weight_sum, weighted = state
    head_count = weighted.shape[0]
    rows = weighted.shape[2]
    normalized = weighted / weight_sum[..., None]
    difference = normalized[:, 0] - lambdas[:, None, None] * normalized[:, 1]
    scale_back = lax.rsqrt(jnp.mean(difference * difference, axis=2, keepdims=True) + NORM_EPS)
    attended = (difference * scale_back * head_gain[None, None, :] * HEAD_KEEP).astype(jnp.bfloat16)
    attended = jnp.transpose(attended, (1, 0, 2)).reshape(rows, head_count * weighted.shape[3])
    row_lse = jnp.transpose(running_max + jnp.log(weight_sum), (2, 0, 1)).reshape(
        rows, 2 * head_count
    )
    return (attended, row_lse)


def project_kernel(scale, tok_ref, gain_ref, wq_ref, wk_ref, wv_ref, cos_ref, sin_ref, q_ref, kv_ref):
    heads, _, pair = q_ref.shape
    width = pair // 2
    widened = tok_ref[...].astype(jnp.float32)
    scaled = (widened * gain_ref[...]).astype(jnp.bfloat16)
    mean = jnp.sum(widened * widened, axis=1, keepdims=True) / widened.shape[1]
    inv_rms = lax.rsqrt(mean + NORM_EPS)
    cosine, sine = cos_ref[...], sin_ref[...]

    def rotary(x):
        return x * cosine + pltpu.roll(x, width // 2, 1) * sine

    q = jnp.dot(scaled, wq_ref[...], preferred_element_type=jnp.float32) * inv_rms
    k = jnp.dot(scaled, wk_ref[...], preferred_element_type=jnp.float32) * inv_rms
    v = jnp.dot(scaled, wv_ref[...], preferred_element_type=jnp.float32) * inv_rms
    for head in range(heads):
        for j in range(2):
            cols = slice((2 * head + j) * width, (2 * head + j + 1) * width)
            place = slice(j * width, (j + 1) * width)
            q_ref[head, :, place] = (rotary(q[:, cols]) * scale).astype(jnp.bfloat16)
            kv_ref[head, :, place] = rotary(k[:, cols]).astype(jnp.bfloat16)
        kv_ref[head, :, pair:] = v[:, head * pair : (head + 1) * pair].astype(jnp.bfloat16)


def project(tokens, norm_gain, w_query, w_key, w_value, positions, head_count, head_width):
    rows, model_width = tokens.shape
    half = head_width // 2
    inverse = ROPE_BASE ** (-jnp.arange(half, dtype=jnp.float32) * 2.0 / head_width)
    angles = positions.astype(jnp.float32)[:, None] * inverse[None, :]
    cosine, sine = jnp.cos(angles), jnp.sin(angles)
    cosine = jnp.concatenate([cosine, cosine], axis=1)
    sine = jnp.concatenate([-sine, sine], axis=1)
    pair = 2 * head_width
    block = rows // 3 if rows % 48 == 0 else rows
    whole = lambda shape: pl.BlockSpec(shape, lambda i: (0,) * len(shape))
    return pl.pallas_call(
        functools.partial(project_kernel, head_width ** (-0.5) * LOG2E),
        grid=(rows // block,),
        out_shape=(
            jax.ShapeDtypeStruct((head_count, rows, pair), jnp.bfloat16),
            jax.ShapeDtypeStruct((head_count, rows, 2 * pair), jnp.bfloat16),
        ),
        in_specs=[
            pl.BlockSpec((block, model_width), lambda i: (i, 0)),
            whole((1, model_width)),
            whole(w_query.shape),
            whole(w_key.shape),
            whole(w_value.shape),
            pl.BlockSpec((block, head_width), lambda i: (i, 0)),
            pl.BlockSpec((block, head_width), lambda i: (i, 0)),
        ],
        out_specs=(
            pl.BlockSpec((head_count, block, pair), lambda i: (0, i, 0)),
            pl.BlockSpec((head_count, block, 2 * pair), lambda i: (0, i, 0)),
        ),
        compiler_params=pltpu.CompilerParams(vmem_limit_bytes=48 * 2**20),
        cost_estimate=pl.CostEstimate(
            flops=6 * rows * model_width * w_query.shape[1],
            bytes_accessed=2 * (rows * model_width + 3 * w_query.size + 3 * rows * w_query.shape[1]),
            transcendentals=0,
        ),
        name="project_qkv",
    )(tokens, norm_gain[None, :], w_query, w_key, w_value, cosine, sine)


def attend_kernel(
    groups,
    block,
    q_keep,
    q_recv,
    kv_keep,
    kv_recv,
    lambdas_ref,
    gain_ref,
    out_ref,
    lse_ref,
    kv_all,
    q_own,
    q_far,
    acc,
    top,
    total,
    local_sem,
    send_right,
    send_left,
    recv_sem,
    far_send,
    far_recv,
):
    sp = lax.axis_index("sp")
    tp = lax.axis_index("tp")
    g, y = sp // 2, sp % 2
    mirror = groups - 1 - g
    rows, pair = q_keep.shape
    width = pair // 2
    blocks = rows // block

    def at(group):
        return (2 * group + y, tp)

    loads = (
        pltpu.make_async_copy(q_keep, q_own.at[y], local_sem.at[0]),
        pltpu.make_async_copy(q_recv, q_own.at[1 - y], local_sem.at[1]),
        pltpu.make_async_copy(kv_keep, kv_all.at[sp], local_sem.at[2]),
        pltpu.make_async_copy(kv_recv, kv_all.at[2 * g + 1 - y], local_sem.at[3]),
    )
    for load in loads:
        load.start()
    barrier = pltpu.get_barrier_semaphore()
    for step in range(1, groups):
        pl.semaphore_signal(
            barrier, inc=1, device_id=at(lax.rem(g + step, groups)), device_id_type=MESH
        )
    pl.semaphore_wait(barrier, groups - 1)
    for load in loads:
        load.wait()

    def right(chunk):
        return pltpu.make_async_remote_copy(
            src_ref=kv_all.at[chunk],
            dst_ref=kv_all.at[chunk],
            send_sem=send_right.at[chunk],
            recv_sem=recv_sem.at[chunk],
            device_id=at(jnp.minimum(g + 1, groups - 1)),
            device_id_type=MESH,
        )

    def left(chunk):
        return pltpu.make_async_remote_copy(
            src_ref=kv_all.at[chunk],
            dst_ref=kv_all.at[chunk],
            send_sem=send_left.at[chunk],
            recv_sem=recv_sem.at[chunk],
            device_id=at(jnp.maximum(g - 1, 0)),
            device_id_type=MESH,
        )

    far = pltpu.make_async_remote_copy(
        src_ref=q_own.at[1],
        dst_ref=q_far,
        send_sem=far_send,
        recv_sem=far_recv,
        device_id=at(mirror),
        device_id_type=MESH,
    )
    far.start()

    @pl.when(g < groups - 1)
    def _():
        right(2 * g + 1).start()
        right(2 * g).start()

    @pl.when(g > 0)
    def _():
        left(2 * g).start()
        left(2 * g + 1).start()

    acc[...] = jnp.zeros_like(acc)
    total[...] = jnp.zeros_like(total)
    top[...] = jnp.full_like(top, MASKED)

    def update(r, j, start, scores, values):
        here = pl.ds(start, block)
        old = top[r, j, here, :]
        new = jnp.maximum(old, jnp.max(scores, axis=1, keepdims=True))
        shrink = jnp.exp2(old - new)
        lifted = jnp.exp2(scores - new[:, :1])
        top[r, j, here, :] = new
        total[r, j, here, :] = shrink * total[r, j, here, :] + jnp.sum(lifted, axis=1, keepdims=True)
        acc[r, j, here, :] = shrink[:, :1] * acc[r, j, here, :] + jnp.dot(
            lifted.astype(jnp.bfloat16), values, preferred_element_type=jnp.float32
        )

    def scores_of(r, j, start, chunk, length):
        cols = slice(j * width, (j + 1) * width)
        queries = q_use[r, pl.ds(start, block), cols]
        keys = kv_all[chunk, :length, cols]
        return lax.dot_general(
            queries, keys, (((1,), (1,)), ((), ())), preferred_element_type=jnp.float32
        )

    q_use = q_own

    def process(r, chunk):
        q_chunk = jnp.where(r == 0, 2 * g, 2 * mirror + 1)

        @pl.when(chunk < q_chunk)
        def _():
            def one(b, carry):
                start = pl.multiple_of(b * block, block)
                for j in range(2):
                    update(r, j, start, scores_of(r, j, start, chunk, rows), kv_all[chunk, :, pair:])
                return carry

            lax.fori_loop(0, blocks, one, 0)

        @pl.when(chunk == q_chunk)
        def _():
            for b in range(blocks):
                length = (b + 1) * block
                query_at = b * block + lax.broadcasted_iota(jnp.int32, (block, length), 0)
                key_at = lax.broadcasted_iota(jnp.int32, (block, length), 1)
                for j in range(2):
                    scores = scores_of(r, j, b * block, chunk, length)
                    scores = jnp.where(key_at <= query_at, scores, MASKED)
                    update(r, j, b * block, scores, kv_all[chunk, :length, pair:])

    far.wait()
    swap = pltpu.make_async_copy(q_far, q_own.at[1], local_sem.at[0])
    swap.start()
    swap.wait()

    def visit(i, carry):
        step, half, side = i // 4, (i // 2) % 2, i % 2
        group = jnp.where(side == 0, g - step, g + step)
        chunk = jnp.where(side == 0, 2 * group + 1 - half, 2 * group + half)
        exists = jnp.logical_and(group >= 0, group < groups)
        exists = jnp.logical_and(exists, jnp.logical_or(step > 0, side == 0))

        @pl.when(exists)
        def _():
            @pl.when(jnp.logical_and(step > 0, side == 0))
            def _():
                right(chunk).wait_recv()

                @pl.when(g < groups - 1)
                def _():
                    right(chunk).start()

            @pl.when(jnp.logical_and(step > 0, side == 1))
            def _():
                left(chunk).wait_recv()

                @pl.when(g > 0)
                def _():
                    left(chunk).start()

            def each(r, inner):
                process(r, chunk)
                return inner

            lax.fori_loop(0, 2, each, 0)

        return carry

    lax.fori_loop(0, 4 * groups, visit, 0)

    lam = lambdas_ref[y]
    gain = gain_ref[...] * HEAD_KEEP

    def close(i, carry):
        r, start = i // blocks, pl.multiple_of((i % blocks) * block, block)
        here = pl.ds(start, block)
        sums = [total[r, j, here, :] for j in range(2)]
        parts = [acc[r, j, here, :] / sums[j][:, :1] for j in range(2)]
        difference = parts[0] - lam * parts[1]
        mean = jnp.mean(difference * difference, axis=1, keepdims=True)
        out_ref[r, here, :] = (difference * lax.rsqrt(mean + NORM_EPS) * gain).astype(jnp.bfloat16)
        lses = [top[r, j, here, :] * (1.0 / LOG2E) + jnp.log(sums[j]) for j in range(2)]
        lane = lax.broadcasted_iota(jnp.int32, lses[0].shape, 1)
        lse_ref[r, here, :] = jnp.where(lane == 0, lses[0], lses[1])
        return carry

    lax.fori_loop(0, 2 * blocks, close, 0)

    def drain(chunk, carry):
        @pl.when(jnp.logical_and(g < groups - 1, chunk < 2 * g + 2))
        def _():
            right(chunk).wait_send()

        @pl.when(jnp.logical_and(g > 0, chunk >= 2 * g))
        def _():
            left(chunk).wait_send()

        return carry

    lax.fori_loop(0, 2 * groups, drain, 0)


def attend(groups, q_keep, q_recv, kv_keep, kv_recv, lambdas, head_gain):
    rows, pair = q_keep.shape
    block = rows // 3 if rows % 48 == 0 else rows
    vmem = pl.BlockSpec(memory_space=pltpu.VMEM)
    anywhere = pl.BlockSpec(memory_space=pl.ANY)
    chunks = 2 * groups
    lanes = 128
    return pl.pallas_call(
        functools.partial(attend_kernel, groups, block),
        out_shape=(
            jax.ShapeDtypeStruct((2, rows, pair), jnp.bfloat16),
            jax.ShapeDtypeStruct((2, rows, lanes), jnp.float32),
        ),
        in_specs=[anywhere] * 4 + [pl.BlockSpec(memory_space=pltpu.SMEM), vmem],
        out_specs=(vmem, vmem),
        scratch_shapes=[
            pltpu.VMEM((chunks, rows, 2 * pair), jnp.bfloat16),
            pltpu.VMEM((2, rows, pair), jnp.bfloat16),
            pltpu.VMEM((rows, pair), jnp.bfloat16),
            pltpu.VMEM((2, 2, rows, pair), jnp.float32),
            pltpu.VMEM((2, 2, rows, lanes), jnp.float32),
            pltpu.VMEM((2, 2, rows, lanes), jnp.float32),
            pltpu.SemaphoreType.DMA((4,)),
            pltpu.SemaphoreType.DMA((chunks,)),
            pltpu.SemaphoreType.DMA((chunks,)),
            pltpu.SemaphoreType.DMA((chunks,)),
            pltpu.SemaphoreType.DMA,
            pltpu.SemaphoreType.DMA,
        ],
        compiler_params=pltpu.CompilerParams(
            collective_id=0, has_side_effects=True, vmem_limit_bytes=56 * 2**20
        ),
        cost_estimate=pl.CostEstimate(
            flops=8 * chunks * rows * rows * 3 * pair // 4,
            bytes_accessed=8 * rows * pair,
            transcendentals=0,
        ),
        name="attend_line",
    )(q_keep, q_recv, kv_keep, kv_recv, lambdas, head_gain[None, :])


def attention_by_head(tokens, norm_gain, w_query, w_key, w_value, lambdas, head_gain, positions):
    head_count = lambdas.shape[0]
    head_width = w_query.shape[1] // (2 * head_count)
    count = lax.axis_size("sp")
    groups = count // 2
    y = lax.axis_index("sp") % 2
    queries, key_values = project(
        tokens, norm_gain, w_query, w_key, w_value, positions, head_count, head_width
    )
    take = lambda array, index: lax.dynamic_index_in_dim(array, index, 0, keepdims=False)
    kv_recv = partner(take(key_values, 1 - y), "sp", 0)
    q_recv = partner(take(queries, 1 - y), "sp", 0)
    result, lse = attend(
        groups, take(queries, y), q_recv, take(key_values, y), kv_recv, lambdas, head_gain
    )
    lse = lse[:, :, :2]
    cross = []
    second = []
    for group in range(groups):
        far = 2 * (groups - 1 - group) + 1
        cross += [(2 * group + 1, 2 * group), (2 * group, far)]
        second += [(2 * group + 1, far)]
    mine = jnp.where(y == 1, result[0], result[1])
    crossed = lax.ppermute(mine, "sp", cross)
    seconded = lax.ppermute(result[1], "sp", second)
    crossed_lse = lax.ppermute(jnp.where(y == 1, lse[0], lse[1]), "sp", cross)
    seconded_lse = lax.ppermute(lse[1], "sp", second)
    first = jnp.where(y == 0, result[0], crossed)
    last = jnp.where(y == 0, crossed, seconded)
    first_lse = jnp.where(y == 0, lse[0], crossed_lse)
    last_lse = jnp.where(y == 0, crossed_lse, seconded_lse)
    return (
        jnp.concatenate([first, last], axis=1),
        jnp.concatenate([first_lse, last_lse], axis=1),
    )


def make_fold(groups, row_count, carry, pieces):
    key_piece, value_piece = pieces
    block_rows = min(key_piece.shape[0], row_count)
    shard_count = key_piece.shape[0] // block_rows

    def one_shard(inner_states, shard_index):
        first_key = shard_index * block_rows
        key_block = lax.dynamic_slice_in_dim(key_piece, shard_index * block_rows, block_rows, 0)
        value_block = lax.dynamic_slice_in_dim(value_piece, shard_index * block_rows, block_rows, 0)
        updated_states = []
        for given_state, group in zip(inner_states, groups):
            group_queries, group_places, group_last = group

            def take_block(given):
                return absorb(given, group_queries, group_places, key_block, value_block, first_key)

            def leave_block(given):
                return given

            updated_states.append(
                lax.cond(first_key < group_last, take_block, leave_block, given_state)
            )
        return (tuple(updated_states), None)

    carry, _ = lax.scan(one_shard, carry, jnp.arange(shard_count, dtype=jnp.int32))
    return carry


def attention_by_rows(query_sums, key_sums, value_sums, lambdas, head_gain, positions):
    row_count = query_sums.shape[0]
    head_count = lambdas.shape[0]
    head_width = query_sums.shape[1] // (2 * head_count)
    offset = lax.axis_index("sp") * row_count
    split = (row_count, 2 * head_count, head_width)
    queries = rotate(query_sums.reshape(split), positions).astype(jnp.bfloat16)
    key_rows = rotate(key_sums.reshape(split), positions).astype(jnp.bfloat16)
    value_rows = value_sums.astype(jnp.bfloat16)
    half_rows = row_count // 2
    bit_count = lax.axis_size("sp").bit_length() - 1
    handed = queries[half_rows:]
    for bit_index in range(bit_count):
        handed = partner(handed, "sp", bit_index)
    mirror = lax.axis_size("sp") - 1 - lax.axis_index("sp")
    mirror_start = mirror * row_count + half_rows
    mirror_places = mirror_start + jnp.arange(half_rows, dtype=jnp.int32)
    groups = (
        (queries[:half_rows], positions[:half_rows], offset + half_rows),
        (handed, mirror_places, mirror_start + half_rows),
    )
    initial = (
        empty_state(head_count, half_rows, head_width),
        empty_state(head_count, half_rows, head_width),
    )
    states = make_fold(
        groups,
        row_count,
        initial,
        (
            lax.all_gather(key_rows, "sp", axis=0, tiled=True),
            lax.all_gather(value_rows, "sp", axis=0, tiled=True),
        ),
    )
    own_attended, own_lse = finish(states[0], lambdas, head_gain)
    answer = finish(states[1], lambdas, head_gain)
    for bit_index in range(bit_count):
        answer = (
            partner(answer[0], "sp", bit_index),
            partner(answer[1].astype(jnp.bfloat16), "sp", bit_index).astype(jnp.float32),
        )
    attended = jnp.concatenate([own_attended, answer[0]], axis=0)
    row_lse = jnp.concatenate([own_lse, answer[1]], axis=0)
    return (attended, row_lse)


def per_device(
    tokens,
    norm_gain,
    w_query,
    w_key,
    w_value,
    w_outer,
    w_inner,
    w_signal,
    conv_taps,
    lambdas,
    head_gain,
    attend_proj,
    convolve_proj,
):
    row_count = tokens.shape[0]
    model_width = norm_gain.shape[0]
    head_count = lambdas.shape[0]
    head_width = w_query.shape[1] // (2 * head_count)
    count = lax.axis_size("sp")
    gathered = lax.all_gather(tokens, "tp", axis=1, tiled=True)
    widened = gathered.astype(jnp.float32)
    scaled = (widened * norm_gain[None, :]).astype(jnp.bfloat16)
    squares = jnp.sum(widened * widened, axis=1)
    inv_rms = lax.rsqrt(squares / model_width + NORM_EPS)[:, None]
    offset = lax.axis_index("sp") * row_count
    positions = offset + jnp.arange(row_count, dtype=jnp.int32)

    def product_of(weight):
        return inv_rms * jnp.dot(scaled, weight, preferred_element_type=jnp.float32)

    if head_count == 2 and head_width == 128 and count % 4 == 0:
        attended, row_lse = attention_by_head(
            gathered, norm_gain, w_query, w_key, w_value, lambdas, head_gain, positions
        )
    else:
        attended, row_lse = attention_by_rows(
            product_of(w_query),
            product_of(w_key),
            product_of(w_value),
            lambdas,
            head_gain,
            positions,
        )
    outer_gate = product_of(w_outer)
    product = product_of(w_inner) * product_of(w_signal)
    border = passed_along(product[row_count - 2 :], "sp", 1)
    padded = jnp.concatenate([border, product], axis=0)
    tap_values = conv_taps.astype(jnp.float32)
    smoothed = (
        tap_values[0] * padded[:-2] + tap_values[1] * padded[1:-1] + tap_values[2] * padded[2:]
    )
    convolved = (outer_gate * smoothed).astype(jnp.bfloat16)
    mixed = lax.psum_scatter(
        (
            jnp.dot(attended, attend_proj, preferred_element_type=jnp.float32)
            + jnp.dot(convolved, convolve_proj, preferred_element_type=jnp.float32)
        ).astype(jnp.bfloat16),
        "tp",
        scatter_dimension=0,
        tiled=True,
    )
    return (mixed, row_lse)


def solution(mesh):
    return jax.shard_map(
        per_device,
        mesh=mesh,
        in_specs=(
            P("sp", "tp"),
            P(),
            P(None, "tp"),
            P(None, "tp"),
            P(None, "tp"),
            P(None, "tp"),
            P(None, "tp"),
            P(None, "tp"),
            P(None, "tp"),
            P("tp"),
            P(),
            P("tp", None),
            P("tp", None),
        ),
        out_specs=(P(("sp", "tp"), None), P("sp", "tp")),
        check_vma=False,
    )
```

```python
import functools
import math

import jax
import jax.numpy as jnp
from jax import lax
from jax.experimental import pallas as pl
from jax.experimental.pallas import tpu as pltpu
from jax.sharding import PartitionSpec as P

ROPE_BASE = 500000.0
NORM_EPS = 1e-05
HEAD_KEEP = 0.8
MASKED = -1e30
LOG2E = math.log2(math.e)
MESH = pl.DeviceIdType.MESH


def partner(value, axis, stride):
    return lax.ppermute(value, axis, [(i, i ^ 1 << stride) for i in range(lax.axis_size(axis))])


def passed_along(value, axis, steps):
    count = lax.axis_size(axis)
    initial, last = (max(0, -steps), min(count, count - steps))
    return lax.ppermute(value, axis, [(source, source + steps) for source in range(initial, last)])


def rotate(values_in, positions):
    half_width = values_in.shape[-1] // 2
    inverse = ROPE_BASE ** (-jnp.arange(half_width, dtype=jnp.float32) * 2.0 / values_in.shape[-1])
    angles = positions.astype(jnp.float32)[:, None] * inverse[None, :]
    cosine = jnp.cos(angles)[:, None, :]
    sine_part = jnp.sin(angles)[:, None, :]
    first_half = values_in[..., :half_width]
    second_half = values_in[..., half_width:]
    return jnp.concatenate(
        [
            first_half * cosine - second_half * sine_part,
            second_half * cosine + first_half * sine_part,
        ],
        axis=-1,
    )


def absorb(state, queries, positions, key_block, value_block, first_key):
    running_max, weight_sum, weighted = state
    head_count = weighted.shape[0]
    block_rows = key_block.shape[0]
    scores = jnp.einsum("qgd,kgd->gqk", queries, key_block, preferred_element_type=jnp.float32)
    scores = scores * queries.shape[-1] ** (-0.5)
    key_places = first_key + jnp.arange(block_rows, dtype=jnp.int32)
    allowed = key_places[None, :] <= positions[:, None]
    scores = jnp.where(allowed[None], scores, MASKED)
    scores = scores.reshape(head_count, 2, positions.shape[0], block_rows)
    raised = jnp.maximum(running_max, jnp.max(scores, axis=3))
    factor = jnp.exp(running_max - raised)
    lifted = jnp.exp(scores - raised[..., None])
    weight_sum = factor * weight_sum + jnp.sum(lifted, axis=3)
    values_here = value_block.reshape(block_rows, head_count, -1)
    weighted = factor[..., None] * weighted + jnp.einsum(
        "hjqk,khe->hjqe",
        lifted.astype(jnp.bfloat16),
        values_here,
        preferred_element_type=jnp.float32,
    )
    return (raised, weight_sum, weighted)


def empty_state(head_count, rows, head_width):
    return (
        jnp.full((head_count, 2, rows), MASKED, jnp.float32),
        jnp.zeros((head_count, 2, rows), jnp.float32),
        jnp.zeros((head_count, 2, rows, 2 * head_width), jnp.float32),
    )


def finish(state, lambdas, head_gain):
    running_max, weight_sum, weighted = state
    head_count = weighted.shape[0]
    rows = weighted.shape[2]
    normalized = weighted / weight_sum[..., None]
    difference = normalized[:, 0] - lambdas[:, None, None] * normalized[:, 1]
    scale_back = lax.rsqrt(jnp.mean(difference * difference, axis=2, keepdims=True) + NORM_EPS)
    attended = (difference * scale_back * head_gain[None, None, :] * HEAD_KEEP).astype(jnp.bfloat16)
    attended = jnp.transpose(attended, (1, 0, 2)).reshape(rows, head_count * weighted.shape[3])
    row_lse = jnp.transpose(running_max + jnp.log(weight_sum), (2, 0, 1)).reshape(
        rows, 2 * head_count
    )
    return (attended, row_lse)


def project_kernel(scale, tok_ref, gain_ref, wq_ref, wk_ref, wv_ref, cos_ref, sin_ref, q_ref, kv_ref):
    heads, _, pair = q_ref.shape
    width = pair // 2
    widened = tok_ref[...].astype(jnp.float32)
    scaled = (widened * gain_ref[...]).astype(jnp.bfloat16)
    mean = jnp.sum(widened * widened, axis=1, keepdims=True) / widened.shape[1]
    inv_rms = lax.rsqrt(mean + NORM_EPS)
    cosine, sine = cos_ref[...], sin_ref[...]

    def rotary(x):
        return x * cosine + pltpu.roll(x, width // 2, 1) * sine

    q = jnp.dot(scaled, wq_ref[...], preferred_element_type=jnp.float32) * inv_rms
    k = jnp.dot(scaled, wk_ref[...], preferred_element_type=jnp.float32) * inv_rms
    v = jnp.dot(scaled, wv_ref[...], preferred_element_type=jnp.float32) * inv_rms
    for head in range(heads):
        for j in range(2):
            cols = slice((2 * head + j) * width, (2 * head + j + 1) * width)
            place = slice(j * width, (j + 1) * width)
            q_ref[head, :, place] = (rotary(q[:, cols]) * scale).astype(jnp.bfloat16)
            kv_ref[head, :, place] = rotary(k[:, cols]).astype(jnp.bfloat16)
        kv_ref[head, :, pair:] = v[:, head * pair : (head + 1) * pair].astype(jnp.bfloat16)


def project(tokens, norm_gain, w_query, w_key, w_value, positions, head_count, head_width):
    rows, model_width = tokens.shape
    half = head_width // 2
    inverse = ROPE_BASE ** (-jnp.arange(half, dtype=jnp.float32) * 2.0 / head_width)
    angles = positions.astype(jnp.float32)[:, None] * inverse[None, :]
    cosine, sine = jnp.cos(angles), jnp.sin(angles)
    cosine = jnp.concatenate([cosine, cosine], axis=1)
    sine = jnp.concatenate([-sine, sine], axis=1)
    pair = 2 * head_width
    block = rows // 3 if rows % 48 == 0 else rows
    whole = lambda shape: pl.BlockSpec(shape, lambda i: (0,) * len(shape))
    return pl.pallas_call(
        functools.partial(project_kernel, head_width ** (-0.5) * LOG2E),
        grid=(rows // block,),
        out_shape=(
            jax.ShapeDtypeStruct((head_count, rows, pair), jnp.bfloat16),
            jax.ShapeDtypeStruct((head_count, rows, 2 * pair), jnp.bfloat16),
        ),
        in_specs=[
            pl.BlockSpec((block, model_width), lambda i: (i, 0)),
            whole((1, model_width)),
            whole(w_query.shape),
            whole(w_key.shape),
            whole(w_value.shape),
            pl.BlockSpec((block, head_width), lambda i: (i, 0)),
            pl.BlockSpec((block, head_width), lambda i: (i, 0)),
        ],
        out_specs=(
            pl.BlockSpec((head_count, block, pair), lambda i: (0, i, 0)),
            pl.BlockSpec((head_count, block, 2 * pair), lambda i: (0, i, 0)),
        ),
        compiler_params=pltpu.CompilerParams(vmem_limit_bytes=48 * 2**20),
        cost_estimate=pl.CostEstimate(
            flops=6 * rows * model_width * w_query.shape[1],
            bytes_accessed=2 * (rows * model_width + 3 * w_query.size + 3 * rows * w_query.shape[1]),
            transcendentals=0,
        ),
        name="project_qkv",
    )(tokens, norm_gain[None, :], w_query, w_key, w_value, cosine, sine)


def attend_kernel(
    groups,
    block,
    q_pair,
    kv_pair,
    lambdas_ref,
    gain_ref,
    out_ref,
    lse_ref,
    kv_all,
    q_own,
    acc,
    top,
    total,
    local_sem,
    send_right,
    recv_sem,
    swap_send,
    swap_recv,
):
    sp = lax.axis_index("sp")
    tp = lax.axis_index("tp")
    g, y = sp // 2, sp % 2
    _, rows, pair = q_pair.shape
    width = pair // 2
    blocks = rows // block

    def at(group, place):
        return (2 * group + place, tp)

    loads = (
        pltpu.make_async_copy(kv_pair.at[y], kv_all.at[sp], local_sem.at[0]),
        pltpu.make_async_copy(q_pair.at[y], q_own.at[y], local_sem.at[1]),
    )
    for load in loads:
        load.start()
    barrier = pltpu.get_barrier_semaphore()
    pl.semaphore_signal(barrier, inc=1, device_id=at(g, 1 - y), device_id_type=MESH)

    @pl.when(g > 0)
    def _():
        pl.semaphore_signal(barrier, inc=1, device_id=at(g - 1, y), device_id_type=MESH)

    @pl.when(g < groups - 1)
    def _():
        pl.semaphore_signal(barrier, inc=1, device_id=at(g + 1, y), device_id_type=MESH)

    beside = jnp.where(g > 0, 1, 0) + jnp.where(g < groups - 1, 1, 0)
    pl.semaphore_wait(barrier, 1 + beside)

    def swap(source, target, index):
        return pltpu.make_async_remote_copy(
            src_ref=source,
            dst_ref=target,
            send_sem=swap_send.at[index],
            recv_sem=swap_recv.at[index],
            device_id=at(g, 1 - y),
            device_id_type=MESH,
        )

    swaps = (
        swap(kv_pair.at[1 - y], kv_all.at[sp], 0),
        swap(q_pair.at[1 - y], q_own.at[y], 1),
    )
    for one_swap in swaps:
        one_swap.start()
    loads[0].wait()

    def right(chunk):
        return pltpu.make_async_remote_copy(
            src_ref=kv_all.at[chunk],
            dst_ref=kv_all.at[chunk],
            send_sem=send_right.at[chunk],
            recv_sem=recv_sem.at[chunk],
            device_id=at(jnp.minimum(g + 1, groups - 1), y),
            device_id_type=MESH,
        )

    @pl.when(g < groups - 1)
    def _():
        right(sp).start()

    acc[...] = jnp.zeros_like(acc)
    total[...] = jnp.zeros_like(total)
    top[...] = jnp.full_like(top, MASKED)

    def update(r, j, start, scores, values):
        here = pl.ds(start, block)
        old = top[r, j, here, :]
        new = jnp.maximum(old, jnp.max(scores, axis=1, keepdims=True))
        shrink = jnp.exp2(old - new)
        lifted = jnp.exp2(scores - new[:, :1])
        top[r, j, here, :] = new
        total[r, j, here, :] = shrink * total[r, j, here, :] + jnp.sum(lifted, axis=1, keepdims=True)
        acc[r, j, here, :] = shrink[:, :1] * acc[r, j, here, :] + jnp.dot(
            lifted.astype(jnp.bfloat16), values, preferred_element_type=jnp.float32
        )

    def scores_of(r, j, start, chunk, length):
        cols = slice(j * width, (j + 1) * width)
        queries = q_own[r, pl.ds(start, block), cols]
        keys = kv_all[chunk, :length, cols]
        return lax.dot_general(
            queries, keys, (((1,), (1,)), ((), ())), preferred_element_type=jnp.float32
        )

    def process(r, chunk):
        q_chunk = 2 * g + r

        @pl.when(chunk < q_chunk)
        def _():
            def one(b, carry):
                start = pl.multiple_of(b * block, block)
                for j in range(2):
                    update(r, j, start, scores_of(r, j, start, chunk, rows), kv_all[chunk, :, pair:])
                return carry

            lax.fori_loop(0, blocks, one, 0)

        @pl.when(chunk == q_chunk)
        def _():
            for b in range(blocks):
                length = (b + 1) * block
                query_at = b * block + lax.broadcasted_iota(jnp.int32, (block, length), 0)
                key_at = lax.broadcasted_iota(jnp.int32, (block, length), 1)
                for j in range(2):
                    scores = scores_of(r, j, b * block, chunk, length)
                    scores = jnp.where(key_at <= query_at, scores, MASKED)
                    update(r, j, b * block, scores, kv_all[chunk, :length, pair:])

    loads[1].wait()
    swaps[0].wait()

    @pl.when(g < groups - 1)
    def _():
        right(2 * g + 1 - y).start()

    swaps[1].wait()

    def visit(i, carry):
        step, half = i // 2, i % 2
        group = g - step
        chunk = 2 * group + jnp.where(half == 0, y, 1 - y)

        @pl.when(step > 0)
        def _():
            right(chunk).wait_recv()

            @pl.when(g < groups - 1)
            def _():
                right(chunk).start()

        def each(r, inner):
            process(r, chunk)
            return inner

        lax.fori_loop(0, 2, each, 0)
        return carry

    lax.fori_loop(0, 2 * g + 2, visit, 0)

    lam = lambdas_ref[y]
    gain = gain_ref[...] * HEAD_KEEP

    def close(i, carry):
        r, start = i // blocks, pl.multiple_of((i % blocks) * block, block)
        here = pl.ds(start, block)
        sums = [total[r, j, here, :] for j in range(2)]
        parts = [acc[r, j, here, :] / sums[j][:, :1] for j in range(2)]
        difference = parts[0] - lam * parts[1]
        mean = jnp.mean(difference * difference, axis=1, keepdims=True)
        out_ref[r, here, :] = (difference * lax.rsqrt(mean + NORM_EPS) * gain).astype(jnp.bfloat16)
        lses = [top[r, j, here, :] * (1.0 / LOG2E) + jnp.log(sums[j]) for j in range(2)]
        lane = lax.broadcasted_iota(jnp.int32, lses[0].shape, 1)
        lse_ref[r, here, :] = jnp.where(lane == 0, lses[0], lses[1])
        return carry

    lax.fori_loop(0, 2 * blocks, close, 0)

    def drain(chunk, carry):
        right(chunk).wait_send()
        return carry

    @pl.when(g < groups - 1)
    def _():
        lax.fori_loop(0, 2 * g + 2, drain, 0)


def attend(groups, q_pair, kv_pair, lambdas, head_gain):
    _, rows, pair = q_pair.shape
    block = rows // 3 if rows % 48 == 0 else rows
    vmem = pl.BlockSpec(memory_space=pltpu.VMEM)
    anywhere = pl.BlockSpec(memory_space=pl.ANY)
    chunks = 2 * groups
    lanes = 128
    return pl.pallas_call(
        functools.partial(attend_kernel, groups, block),
        out_shape=(
            jax.ShapeDtypeStruct((2, rows, pair), jnp.bfloat16),
            jax.ShapeDtypeStruct((2, rows, lanes), jnp.float32),
        ),
        in_specs=[anywhere] * 2 + [pl.BlockSpec(memory_space=pltpu.SMEM), vmem],
        out_specs=(vmem, vmem),
        scratch_shapes=[
            pltpu.VMEM((chunks, rows, 2 * pair), jnp.bfloat16),
            pltpu.VMEM((2, rows, pair), jnp.bfloat16),
            pltpu.VMEM((2, 2, rows, pair), jnp.float32),
            pltpu.VMEM((2, 2, rows, lanes), jnp.float32),
            pltpu.VMEM((2, 2, rows, lanes), jnp.float32),
            pltpu.SemaphoreType.DMA((2,)),
            pltpu.SemaphoreType.DMA((chunks,)),
            pltpu.SemaphoreType.DMA((chunks,)),
            pltpu.SemaphoreType.DMA((2,)),
            pltpu.SemaphoreType.DMA((2,)),
        ],
        compiler_params=pltpu.CompilerParams(
            collective_id=0, has_side_effects=True, vmem_limit_bytes=56 * 2**20
        ),
        cost_estimate=pl.CostEstimate(
            flops=8 * chunks * rows * rows * 3 * pair // 4,
            bytes_accessed=8 * rows * pair,
            transcendentals=0,
        ),
        name="attend_line",
    )(q_pair, kv_pair, lambdas, head_gain[None, :])


def attention_by_head(tokens, norm_gain, w_query, w_key, w_value, lambdas, head_gain, positions):
    head_count = lambdas.shape[0]
    head_width = w_query.shape[1] // (2 * head_count)
    count = lax.axis_size("sp")
    groups = count // 2
    y = lax.axis_index("sp") % 2
    queries, key_values = project(
        tokens, norm_gain, w_query, w_key, w_value, positions, head_count, head_width
    )
    result, lse = attend(groups, queries, key_values, lambdas, head_gain)
    lse = lse[:, :, :2]
    at_first = y == 0
    crossed = partner(jnp.where(at_first, result[1], result[0]), "sp", 0)
    crossed_lse = partner(jnp.where(at_first, lse[1], lse[0]), "sp", 0)
    first = jnp.where(at_first, result[0], crossed)
    last = jnp.where(at_first, crossed, result[1])
    first_lse = jnp.where(at_first, lse[0], crossed_lse)
    last_lse = jnp.where(at_first, crossed_lse, lse[1])
    return (
        jnp.concatenate([first, last], axis=1),
        jnp.concatenate([first_lse, last_lse], axis=1),
    )


def make_fold(groups, row_count, carry, pieces):
    key_piece, value_piece = pieces
    block_rows = min(key_piece.shape[0], row_count)
    shard_count = key_piece.shape[0] // block_rows

    def one_shard(inner_states, shard_index):
        first_key = shard_index * block_rows
        key_block = lax.dynamic_slice_in_dim(key_piece, shard_index * block_rows, block_rows, 0)
        value_block = lax.dynamic_slice_in_dim(value_piece, shard_index * block_rows, block_rows, 0)
        updated_states = []
        for given_state, group in zip(inner_states, groups):
            group_queries, group_places, group_last = group

            def take_block(given):
                return absorb(given, group_queries, group_places, key_block, value_block, first_key)

            def leave_block(given):
                return given

            updated_states.append(
                lax.cond(first_key < group_last, take_block, leave_block, given_state)
            )
        return (tuple(updated_states), None)

    carry, _ = lax.scan(one_shard, carry, jnp.arange(shard_count, dtype=jnp.int32))
    return carry


def attention_by_rows(query_sums, key_sums, value_sums, lambdas, head_gain, positions):
    row_count = query_sums.shape[0]
    head_count = lambdas.shape[0]
    head_width = query_sums.shape[1] // (2 * head_count)
    offset = lax.axis_index("sp") * row_count
    split = (row_count, 2 * head_count, head_width)
    queries = rotate(query_sums.reshape(split), positions).astype(jnp.bfloat16)
    key_rows = rotate(key_sums.reshape(split), positions).astype(jnp.bfloat16)
    value_rows = value_sums.astype(jnp.bfloat16)
    half_rows = row_count // 2
    bit_count = lax.axis_size("sp").bit_length() - 1
    handed = queries[half_rows:]
    for bit_index in range(bit_count):
        handed = partner(handed, "sp", bit_index)
    mirror = lax.axis_size("sp") - 1 - lax.axis_index("sp")
    mirror_start = mirror * row_count + half_rows
    mirror_places = mirror_start + jnp.arange(half_rows, dtype=jnp.int32)
    groups = (
        (queries[:half_rows], positions[:half_rows], offset + half_rows),
        (handed, mirror_places, mirror_start + half_rows),
    )
    initial = (
        empty_state(head_count, half_rows, head_width),
        empty_state(head_count, half_rows, head_width),
    )
    states = make_fold(
        groups,
        row_count,
        initial,
        (
            lax.all_gather(key_rows, "sp", axis=0, tiled=True),
            lax.all_gather(value_rows, "sp", axis=0, tiled=True),
        ),
    )
    own_attended, own_lse = finish(states[0], lambdas, head_gain)
    answer = finish(states[1], lambdas, head_gain)
    for bit_index in range(bit_count):
        answer = (
            partner(answer[0], "sp", bit_index),
            partner(answer[1].astype(jnp.bfloat16), "sp", bit_index).astype(jnp.float32),
        )
    attended = jnp.concatenate([own_attended, answer[0]], axis=0)
    row_lse = jnp.concatenate([own_lse, answer[1]], axis=0)
    return (attended, row_lse)


def per_device(
    tokens,
    norm_gain,
    w_query,
    w_key,
    w_value,
    w_outer,
    w_inner,
    w_signal,
    conv_taps,
    lambdas,
    head_gain,
    attend_proj,
    convolve_proj,
):
    row_count = tokens.shape[0]
    model_width = norm_gain.shape[0]
    head_count = lambdas.shape[0]
    head_width = w_query.shape[1] // (2 * head_count)
    count = lax.axis_size("sp")
    gathered = lax.all_gather(tokens, "tp", axis=1, tiled=True)
    widened = gathered.astype(jnp.float32)
    scaled = (widened * norm_gain[None, :]).astype(jnp.bfloat16)
    squares = jnp.sum(widened * widened, axis=1)
    inv_rms = lax.rsqrt(squares / model_width + NORM_EPS)[:, None]
    offset = lax.axis_index("sp") * row_count
    positions = offset + jnp.arange(row_count, dtype=jnp.int32)

    def product_of(weight):
        return inv_rms * jnp.dot(scaled, weight, preferred_element_type=jnp.float32)

    if head_count == 2 and head_width == 128 and count % 2 == 0:
        attended, row_lse = attention_by_head(
            gathered, norm_gain, w_query, w_key, w_value, lambdas, head_gain, positions
        )
    else:
        attended, row_lse = attention_by_rows(
            product_of(w_query),
            product_of(w_key),
            product_of(w_value),
            lambdas,
            head_gain,
            positions,
        )
    outer_gate = product_of(w_outer)
    product = product_of(w_inner) * product_of(w_signal)
    border = passed_along(product[row_count - 2 :], "sp", 1)
    padded = jnp.concatenate([border, product], axis=0)
    tap_values = conv_taps.astype(jnp.float32)
    smoothed = (
        tap_values[0] * padded[:-2] + tap_values[1] * padded[1:-1] + tap_values[2] * padded[2:]
    )
    convolved = (outer_gate * smoothed).astype(jnp.bfloat16)
    mixed = lax.psum_scatter(
        (
            jnp.dot(attended, attend_proj, preferred_element_type=jnp.float32)
            + jnp.dot(convolved, convolve_proj, preferred_element_type=jnp.float32)
        ).astype(jnp.bfloat16),
        "tp",
        scatter_dimension=0,
        tiled=True,
    )
    return (mixed, row_lse)


def solution(mesh):
    return jax.shard_map(
        per_device,
        mesh=mesh,
        in_specs=(
            P("sp", "tp"),
            P(),
            P(None, "tp"),
            P(None, "tp"),
            P(None, "tp"),
            P(None, "tp"),
            P(None, "tp"),
            P(None, "tp"),
            P(None, "tp"),
            P("tp"),
            P(),
            P("tp", None),
            P("tp", None),
        ),
        out_specs=(P(("sp", "tp"), None), P("sp", "tp")),
        check_vma=False,
    )
```
